32 devices in a mesh: sp: 8 (over z, y), tp: 4 (over x, core).
Axes of the slice: x: 2, y: 2, z: 4, core: 2. Of those that a mesh axis runs over, the one named last changes fastest.
Arguments:
- inputs: bfloat16 [8192, 2048], P(('sp', 'tp')), may hold values from -90 to 90
- in_gain: float32 [2048], replicated, may hold values from 0.1 to 1.9
- w_query: bfloat16 [2048, 1024], replicated, may hold values from -2 to 2
- w_key: bfloat16 [2048, 128], replicated, may hold values from -2 to 2
- w_value: bfloat16 [2048, 128], replicated, may hold values from -0.125 to 0.125
- query_gain: float32 [64], replicated, may hold values from 0 to 8, as said below
- key_gain: float32 [64], replicated, may hold values from 0 to 8, as said below
- decay_sums: float32 [8192, 16], P('sp', 'tp'), may hold values from -1173 to 0, as said below
- w_out: bfloat16 [1024, 2048], replicated, may hold values from -0.1875 to 0.1875
Outputs:
- result: bfloat16 [8192, 2048], P(('sp', 'tp'))
The draws below stay inside these ranges and needn't reach their ends.
Inputs may be any that keep to these rules, and one draw needn't show every extreme that they name: `decay_sums`: along positions, each head's entries never rise. `query_gain`: every entry is positive. `key_gain`: every entry is positive.
All inputs are finite; a program needn't handle non-finite values.
Results may differ from the reference program's by a relative error of at most 0.015.
The reference program's roundings to bfloat16 on the way count: a program that leaves them out, or rounds other values in their place, can miss the bound.
Values may be sent and summed in bfloat16 or wider, within the bound.
No kernel may reach another device: no remote copies, remote signals or barrier semaphores. Data moves between devices by JAX's collectives and lax.ppermute only.
A program may use at most 64 MiB of HBM per device.

```python
import math
import jax
import jax.numpy as jnp
from jax import lax

D = 2048
QUERY_HEADS = 16
DH = 64
KV = 2
TOK_DEV = 1024
SEQUENCE_LENGTH = 8192


def draw_inputs(key, part):
    key_noise, key_shift = jax.random.split(jax.random.fold_in(key, 13), 2)
    noise = jax.random.truncated_normal(key_noise, -5.0, 5.0, (SEQUENCE_LENGTH, D), jnp.float32)
    shift = jax.random.truncated_normal(key_shift, -4.0, 4.0, (SEQUENCE_LENGTH // TOK_DEV, D), jnp.float32)
    shifted = noise + jnp.repeat(shift, TOK_DEV, axis=0)
    return shifted.astype(jnp.bfloat16)


def draw_w_query(key, part):
    noise = jax.random.truncated_normal(jax.random.fold_in(key, 31), -6.0, 6.0, (D, QUERY_HEADS * DH), jnp.float32) * D ** (-0.5)
    return noise.astype(jnp.bfloat16)


def draw_w_key(key, part):
    noise = jax.random.truncated_normal(jax.random.fold_in(key, 32), -6.0, 6.0, (D, KV * DH), jnp.float32) * D ** (-0.5)
    return noise.astype(jnp.bfloat16)


def draw_query_gain(key, part):
    return jax.random.uniform(jax.random.fold_in(key, 11), (DH,), jnp.float32, 0.4, 1.6)


def draw_key_gain(key, part):
    return jax.random.uniform(jax.random.fold_in(key, 12), (DH,), jnp.float32, 0.4, 1.6)


def draw_decay_sums(key, part):
    random_part_keys = jax.random.split(jax.random.fold_in(key, 14), 7)
    order = jax.random.permutation(random_part_keys[0], QUERY_HEADS)
    fast_count = QUERY_HEADS // 2
    fast = (order < fast_count)[None, :]
    slow_rate = jax.random.uniform(random_part_keys[1], (1, QUERY_HEADS), jnp.float32, 0.2, 0.6) / SEQUENCE_LENGTH
    fast_rate = jax.random.uniform(random_part_keys[2], (1, QUERY_HEADS), jnp.float32, 1.0 / 60.0, 1.0 / 25.0)
    base_offset = jnp.where(fast, fast_rate, slow_rate)
    coarse_estimate = jax.random.uniform(random_part_keys[3], (SEQUENCE_LENGTH, QUERY_HEADS), jnp.float32, 0.3, 1.7)
    block_multiple = jnp.exp(jax.random.uniform(random_part_keys[4], (SEQUENCE_LENGTH // TOK_DEV, QUERY_HEADS), jnp.float32, -math.log(2.0), math.log(2.0)))
    block_multiple = jnp.repeat(block_multiple, TOK_DEV, axis=0)
    spike_position = jax.random.randint(random_part_keys[5], (3,), 0, SEQUENCE_LENGTH)
    spike_depth = jnp.log(jax.random.uniform(random_part_keys[6], (3, QUERY_HEADS), jnp.float32, 0.5, 0.8))
    match_count = (jnp.arange(SEQUENCE_LENGTH, dtype=jnp.int32)[:, None] == spike_position[None, :]).astype(jnp.float32)
    spike_list = jnp.dot(match_count, spike_depth, precision=lax.Precision.HIGHEST)
    step_log_gates = -base_offset * coarse_estimate * block_multiple + spike_list
    return jnp.cumsum(step_log_gates, axis=0)


def gaussian(rng, shape, spread, most, kind=jnp.bfloat16):
    drawn = jax.random.normal(rng, shape, jnp.float32) * spread
    return jnp.minimum(jnp.maximum(drawn, -most), most).astype(kind)


def setup_inputs(seed: int = 0) -> dict:
    arg_keys = jax.random.split(jax.random.key(seed), 10)
    inputs = draw_inputs(jax.random.fold_in(arg_keys[9], 71), 0)
    in_gain = jnp.clip(1.0 + 0.18 * jax.random.normal(arg_keys[1], (D,), jnp.float32), 0.1, 1.9)
    w_query = draw_w_query(jax.random.fold_in(arg_keys[9], 71), 0)
    w_key = draw_w_key(jax.random.fold_in(arg_keys[9], 71), 0)
    w_value = gaussian(arg_keys[4], (D, KV * DH), D ** -0.5, 0.125)
    query_gain = draw_query_gain(jax.random.fold_in(arg_keys[9], 71), 0)
    key_gain = draw_key_gain(jax.random.fold_in(arg_keys[9], 71), 0)
    decay_sums = draw_decay_sums(jax.random.fold_in(arg_keys[9], 71), 0)
    w_out = gaussian(arg_keys[8], (QUERY_HEADS * DH, D), (QUERY_HEADS * DH) ** -0.5, 0.1875)
    return dict(inputs=inputs, in_gain=in_gain, w_query=w_query, w_key=w_key, w_value=w_value, query_gain=query_gain, key_gain=key_gain, decay_sums=decay_sums, w_out=w_out)


epsilon = 1e-06

def rms_norm(vector, gain_vec):
    return vector * lax.rsqrt(lax.optimization_barrier(jnp.mean(vector * vector, axis=-1, keepdims=True)) + epsilon) * gain_vec

def reference(inputs, in_gain, w_query, w_key, w_value, query_gain, key_gain, decay_sums, w_out):
    length = inputs.shape[0]
    normed = rms_norm(inputs.astype(jnp.float32), in_gain).astype(jnp.bfloat16)
    queries = rms_norm(jnp.dot(normed, w_query, preferred_element_type=jnp.float32).reshape(length, QUERY_HEADS, DH), query_gain).astype(jnp.bfloat16)
    keys = rms_norm(jnp.dot(normed, w_key, preferred_element_type=jnp.float32).reshape(length, KV, DH), key_gain).astype(jnp.bfloat16)
    values = jnp.dot(normed, w_value, preferred_element_type=jnp.float32).astype(jnp.bfloat16).reshape(length, KV, DH)
    group_size = QUERY_HEADS // KV
    keys_wide = jnp.repeat(keys, group_size, axis=1).astype(jnp.float32)
    values_wide = jnp.repeat(values, group_size, axis=1).astype(jnp.float32)
    block_rows = math.gcd(length, 512)
    block_count = length // block_rows
    key_pos = jnp.arange(length, dtype=jnp.int32)
    key_decay = decay_sums.T
    score_scale = DH ** (-0.5)

    def attend_block(block_index):
        offset = (block_index * block_rows).astype(jnp.int32)
        query_rows = lax.dynamic_slice_in_dim(queries, offset, block_rows, 0).astype(jnp.float32)
        query_decay = lax.dynamic_slice_in_dim(decay_sums, offset, block_rows, 0)
        scores = jnp.einsum('qhd,khd->hqk', query_rows, keys_wide) * score_scale
        scores = scores + query_decay.T[:, :, None] - key_decay[:, None, :]
        query_pos = offset + jnp.arange(block_rows, dtype=jnp.int32)
        visible = key_pos[None, :] <= query_pos[:, None]
        scores = jnp.where(visible[None], scores, -1e+30)
        peak = lax.optimization_barrier(jnp.max(scores, axis=-1, keepdims=True))
        weights_exp = jnp.where(visible[None], jnp.exp(scores - peak), 0.0)
        total = lax.optimization_barrier(jnp.sum(weights_exp, axis=-1))
        rounded = lax.optimization_barrier(weights_exp.astype(jnp.bfloat16)).astype(jnp.float32)
        mixed = jnp.einsum('hqk,khd->qhd', rounded, values_wide)
        return (mixed / total.T[:, :, None]).astype(jnp.bfloat16)
    blocks = lax.map(attend_block, jnp.arange(block_count, dtype=jnp.int32))
    attended = blocks.reshape(length, QUERY_HEADS * DH)
    return jnp.dot(attended, w_out, preferred_element_type=jnp.float32).astype(jnp.bfloat16)
```

```python
from functools import partial
import math

import jax
import jax.numpy as jnp
from jax import lax
from jax.experimental import pallas as pl
from jax.experimental.pallas import tpu as pltpu
from jax.sharding import PartitionSpec as P

epsilon = 1e-06
LOG2E = math.log2(math.e)
SAFE_SCORE = 60.0
W = 256
LAG = 2
OUT_LAG = 2


def rms_norm(vector, gain_vec):
    return (
        vector * lax.rsqrt(jnp.mean(vector * vector, axis=-1, keepdims=True) + epsilon) * gain_vec
    )


def three_way(x):
    hi = x.astype(jnp.bfloat16)
    rest = x - hi.astype(jnp.float32)
    mid = rest.astype(jnp.bfloat16)
    lo = (rest - mid.astype(jnp.float32)).astype(jnp.bfloat16)
    return hi, mid, lo


def attend_kernel(dims, *refs):
    sp, tp, rows, half, heads_dev, group_heads, head_size = dims
    n_piece = sp * half
    scal = refs[0]
    kv_refs = refs[1 : 1 + n_piece]
    dec_refs = refs[1 + n_piece : 1 + n_piece + sp // 2]
    q_own, q_recv = refs[1 + n_piece + sp // 2 : 3 + n_piece + sp // 2]
    o_own, o_other = refs[3 + n_piece + sp // 2 : 5 + n_piece + sp // 2]
    keys, vals, qs, acc, tot, dq, peak, outs = refs[5 + n_piece + sp // 2 :]
    tok = tp * rows
    s_rank, c_rank, g_rank, unsafe = scal[0], scal[1], scal[2], scal[3]
    tiles = acc.shape[0]
    pairs = tiles // 2
    n_key = tok // W
    cols = 2 * rows
    bf16, f32 = jnp.bfloat16, jnp.float32

    for k in range(sp // 2):
        for yy in range(2):
            blk = scal[4 + 2 * k + yy]

            @pl.when(blk <= s_rank)
            def _(k=k, yy=yy, blk=blk):
                for j in range(half):
                    member = lax.rem(c_rank - j + half, half)
                    src = kv_refs[(2 * k + yy) * half + j]
                    for hf in range(2):
                        chunk = (member + hf * half) * rows
                        base = pl.multiple_of(blk * tok + chunk, 128)
                        for u in range(rows // 128):
                            kv = src[hf * rows + u * 128 : hf * rows + (u + 1) * 128, :]
                            kv_t = kv.T
                            lane = pl.multiple_of(yy * tok + chunk + u * 128, 128)
                            dec = dec_refs[k][:, pl.ds(lane, 128)]
                            hi, mid, lo = three_way(dec)
                            ones = jnp.ones(dec.shape, f32)
                            extra = jnp.concatenate(
                                [
                                    kv_t[:head_size].astype(f32),
                                    hi.astype(f32),
                                    mid.astype(f32),
                                    lo.astype(f32),
                                    ones,
                                    jnp.zeros((128 - head_size - 32, 128), f32),
                                ],
                                axis=0,
                            )
                            dst = pl.multiple_of(base + u * 128, 128)
                            keys[pl.ds(dst, 128), :128] = kv
                            keys[pl.ds(dst, 128), 128:] = extra.T.astype(bf16)
                            vals[:, pl.ds(dst, 128)] = kv_t[head_size:]

    q0 = jnp.where(g_rank == 0, q_own[...], q_recv[...])
    q1 = jnp.where(g_rank == 0, q_recv[...], q_own[...])
    row8 = lax.broadcasted_iota(jnp.int32, (8, cols), 0)
    for h in range(group_heads):
        qc = jnp.concatenate(
            [q0[h * head_size : (h + 1) * head_size], q1[h * head_size : (h + 1) * head_size]],
            axis=1,
        ).astype(f32) * (LOG2E * head_size**-0.5)
        q_hi = qc.astype(bf16)
        q_lo = (qc - q_hi.astype(f32)).astype(bf16)
        dec_row = lax.rem(c_rank - h // heads_dev + half, half) * heads_dev + h % heads_dev
        pick = jnp.where(row8 == dec_row, -1.0, 0.0).astype(f32)
        d_lo = dec_refs[0][:, pl.ds(pl.multiple_of(c_rank * rows, 128), rows)]
        d_hi = dec_refs[0][:, pl.ds(pl.multiple_of((c_rank + half) * rows, 128), rows)]
        own = -jnp.sum(jnp.concatenate([d_lo, d_hi], axis=1) * pick, axis=0, keepdims=True)
        d1, d2, d3 = three_way(own)
        own8 = jnp.where(
            row8 == 0,
            d1.astype(f32),
            jnp.where(row8 == 1, d2.astype(f32), jnp.where(row8 == 2, d3.astype(f32), 0.0)),
        )
        tail = jnp.concatenate(
            [pick, pick, pick, own8, jnp.zeros((W - 192 - 32, cols), f32)], axis=0
        ).astype(bf16)
        for v in range(cols // W):
            n = h * (cols // W) + v
            sl = slice(v * W, (v + 1) * W)
            qs[n, 0:64] = q_hi[:, sl]
            qs[n, 64:128] = jnp.zeros((64, W), bf16)
            qs[n, 128:192] = q_lo[:, sl]
            qs[n, 192:256] = tail[:, sl]
            dq[n] = own[:, sl]

    acc[...] = jnp.zeros_like(acc)
    tot[...] = jnp.zeros_like(tot)

    def q_pos(n):
        flat = (n * W) % cols + lax.broadcasted_iota(jnp.int32, (1, W), 1)
        side = flat // rows
        return (c_rank + side * half) * rows + (flat - side * rows)

    def scoped(*accs):
        ring = LAG + 1
        per = ring + 2
        s_acc = [accs[m * per : m * per + ring] for m in range(2)]
        o_acc = [accs[m * per + ring : m * per + per] for m in range(2)]

        @pl.when(unsafe == 1)
        def _():
            peak[...] = jnp.full(peak.shape, -1e30, f32)

            def tile_max(n, carry):
                def block_max(b, carry):
                    off = pl.multiple_of(b * W, W)
                    pltpu.matmul_push_rhs(qs[n], staging_register=0, mxu_index=0)
                    pltpu.matmul_acc_lhs(s_acc[0][0], keys[pl.ds(off, W), :], load_staged_rhs=0)
                    s = pltpu.matmul_pop(s_acc[0][0])
                    k_pos = off + lax.broadcasted_iota(jnp.int32, (W, W), 0)
                    flat = lax.rem(n * W, cols) + lax.broadcasted_iota(jnp.int32, (1, W), 1)
                    side = flat // rows
                    pos = s_rank * tok + (c_rank + side * half) * rows + (flat - side * rows)
                    s = jnp.where(k_pos <= pos, s, -1e30)
                    peak[n] = jnp.maximum(peak[n], jnp.max(s, axis=0, keepdims=True))
                    return carry

                lax.fori_loop(0, (s_rank + 1) * n_key, block_max, 0)
                d1, d2, d3 = three_way(dq[n] - peak[n])
                r16 = lax.broadcasted_iota(jnp.int32, (16, W), 0)
                old = qs[n, 208:224].astype(f32)
                new = jnp.where(
                    r16 == 8,
                    d1.astype(f32),
                    jnp.where(
                        r16 == 9, d2.astype(f32), jnp.where(r16 == 10, d3.astype(f32), old)
                    ),
                )
                qs[n, 208:224] = new.astype(bf16)
                return carry

            lax.fori_loop(0, tiles, tile_max, 0)

        def block(i, masked):
            steps = [(p, kb) for p in range(pairs) for kb in range(n_key)]
            start = pl.multiple_of(i * tok, W)

            def front(n):
                p, kb = steps[n]
                kk = keys[pl.ds(start + kb * W, W), :]
                for m in range(2):
                    pltpu.matmul_push_rhs(qs[2 * p + m], staging_register=0, mxu_index=m)
                    pltpu.matmul_acc_lhs(s_acc[m][n % ring], kk, load_staged_rhs=0)

            def back(n):
                p, kb = steps[n]
                vt = vals[:, pl.ds(start + kb * W, W)]
                for m in range(2):
                    e = jnp.exp2(pltpu.matmul_pop(s_acc[m][n % ring]))
                    if masked:
                        k_pos = kb * W + lax.broadcasted_iota(jnp.int32, (W, W), 0)
                        e = jnp.where(k_pos <= q_pos(2 * p + m), e, 0.0)
                    tot[2 * p + m] += jnp.sum(e.reshape(W // 8, 8, W), axis=0)
                    pltpu.matmul_push_rhs(e.astype(bf16), staging_register=1, mxu_index=m)
                    pltpu.matmul_acc_lhs(o_acc[m][p % 2], vt, load_staged_rhs=1)

            def finish(n):
                p, kb = steps[n]
                if kb == n_key - 1:
                    for m in range(2):
                        acc[2 * p + m] += pltpu.matmul_pop(o_acc[m][p % 2])

            total_steps = len(steps)
            for n in range(total_steps + LAG + OUT_LAG):
                if n < total_steps:
                    front(n)
                if LAG <= n < total_steps + LAG:
                    back(n - LAG)
                if n >= LAG + OUT_LAG:
                    finish(n - LAG - OUT_LAG)

        def full_block(i, carry):
            block(i, False)
            return carry

        lax.fori_loop(0, s_rank, full_block, 0)
        block(s_rank, True)

    specs = []
    for m in range(2):
        specs += [pltpu.ACC(m)((W, W), f32)] * (LAG + 1) + [pltpu.ACC(m)((head_size, W), f32)] * 2
    pl.run_scoped(scoped, *specs)

    for n in range(tiles):
        h, v = n // (cols // W), n % (cols // W)
        value = acc[n] / jnp.sum(tot[n], axis=0, keepdims=True)
        outs[h * head_size : (h + 1) * head_size, v * W : (v + 1) * W] = value.astype(bf16)
    side0, side1 = outs[:, :rows], outs[:, rows:]
    o_own[...] = jnp.where(g_rank == 0, side0, side1)
    o_other[...] = jnp.where(g_rank == 0, side1, side0)


def ring_next(count):
    order = [0] + list(range(1, count, 2)) + list(range((count - 1) // 2 * 2, 0, -2))
    return {order[i]: order[(i + 1) % count] for i in range(count)}, order


def per_device(inputs, in_gain, w_query, w_key, w_value, query_gain, key_gain, decay_sums, w_out):
    tp, sp = lax.axis_size("tp"), lax.axis_size("sp")
    s_rank, t_rank = lax.axis_index("sp"), lax.axis_index("tp")
    heads_dev = decay_sums.shape[1]
    head_size = query_gain.shape[0]
    kv_heads = w_key.shape[1] // head_size
    half = tp // kv_heads
    g_rank, c_rank = t_rank // half, t_rank % half
    group_heads = heads_dev * half
    rows = inputs.shape[0]
    tok = rows * tp
    bf16, f32 = jnp.bfloat16, jnp.float32
    axes = ("sp", "tp")
    zs = sp // 2

    def move(array, target):
        pairs = []
        for s in range(sp):
            for t in range(tp):
                s2, t2 = target(s, t)
                pairs.append((s * tp + t, s2 * tp + t2))
        return lax.ppermute(array, axes, pairs)

    nxt, order = ring_next(zs)
    to_x = lambda s, t: (s, (t + half) % tp)
    to_y = lambda s, t: (s ^ 1, t)
    to_z = lambda s, t: (nxt[s // 2] * 2 + s % 2, t)

    def to_core(j):
        return lambda s, t: (s, t // half * half + (t % half + j) % half)

    dec = (decay_sums * LOG2E).T
    dec = jnp.concatenate([dec] + [move(dec, to_core(j)) for j in range(1, half)], axis=0)
    dec = jnp.concatenate([dec, move(dec, to_y)], axis=1)
    decs = [dec]
    for _ in range(zs - 1):
        decs.append(move(decs[-1], to_z))

    normed = rms_norm(inputs.astype(f32), in_gain).astype(bf16)
    key_all = rms_norm(
        jnp.dot(normed, w_key, preferred_element_type=f32).reshape(rows, kv_heads, head_size),
        key_gain,
    ).astype(bf16)
    value_all = (
        jnp.dot(normed, w_value, preferred_element_type=f32)
        .astype(bf16)
        .reshape(rows, kv_heads, head_size)
    )
    pair = jnp.concatenate([key_all, value_all], axis=2)
    mine = jnp.where(g_rank == 0, pair[:, 0], pair[:, 1])
    theirs = move(jnp.where(g_rank == 0, pair[:, 1], pair[:, 0]), to_x)
    own = jnp.concatenate(
        [jnp.where(g_rank == 0, mine, theirs), jnp.where(g_rank == 0, theirs, mine)], axis=0
    )
    pieces = []
    for k in range(zs):
        if k:
            own = move(own, to_z)
        side = move(own, to_y)
        for part in (own, side):
            pieces += [part] + [move(part, to_core(j)) for j in range(1, half)]

    query_all = rms_norm(
        jnp.dot(normed, w_query, preferred_element_type=f32).reshape(
            rows, kv_heads * group_heads, head_size
        ),
        query_gain,
    ).astype(bf16)
    query_t = query_all.reshape(rows, kv_heads, group_heads * head_size).transpose(1, 2, 0)
    q_own = jnp.where(g_rank == 0, query_t[0], query_t[1])
    q_recv = move(jnp.where(g_rank == 0, query_t[1], query_t[0]), to_x)

    source = jnp.array(
        [[order[(order.index(z) - k) % zs] for k in range(zs)] for z in range(zs)], jnp.int32
    )[s_rank // 2]
    y_rank = s_rank % 2
    blocks = jnp.stack([source * 2 + y_rank, source * 2 + (1 - y_rank)], axis=1).reshape(-1)
    bound = jnp.max(query_gain * key_gain) * (head_size**0.5 * 1.02)
    unsafe = jnp.where(bound <= SAFE_SCORE, 0, 1).astype(jnp.int32)
    scal = jnp.concatenate(
        [jnp.stack([s_rank, c_rank, g_rank, unsafe]).astype(jnp.int32), blocks.astype(jnp.int32)]
    )

    width = group_heads * head_size
    tiles = group_heads * 2 * rows // W
    vmem = pl.BlockSpec(memory_space=pltpu.VMEM)
    att_own, att_other = pl.pallas_call(
        partial(attend_kernel, (sp, tp, rows, half, heads_dev, group_heads, head_size)),
        out_shape=[jax.ShapeDtypeStruct((width, rows), bf16)] * 2,
        in_specs=[pl.BlockSpec(memory_space=pltpu.SMEM)] + [vmem] * (len(pieces) + len(decs) + 2),
        out_specs=[vmem] * 2,
        scratch_shapes=[
            pltpu.VMEM((sp * tok, W), bf16),
            pltpu.VMEM((head_size, sp * tok), bf16),
            pltpu.VMEM((tiles, W, W), bf16),
            pltpu.VMEM((tiles, head_size, W), f32),
            pltpu.VMEM((tiles, 8, W), f32),
            pltpu.VMEM((tiles, 1, W), f32),
            pltpu.VMEM((tiles, 1, W), f32),
            pltpu.VMEM((width, 2 * rows), bf16),
        ],
        compiler_params=pltpu.CompilerParams(vmem_limit_bytes=48 * 2**20),
        cost_estimate=pl.CostEstimate(
            flops=4 * 2 * rows * group_heads * sp * tok * head_size,
            bytes_accessed=sp * tok * 4 * head_size,
            transcendentals=2 * rows * group_heads * sp * tok,
        ),
        name="attend",
    )(scal, *pieces, *decs, q_own, q_recv)
    back = move(att_other, to_x)
    att = jnp.concatenate(
        [jnp.where(g_rank == 0, att_own, back), jnp.where(g_rank == 0, back, att_own)], axis=0
    )
    return lax.dot_general(
        att, w_out, (((0,), (0,)), ((), ())), preferred_element_type=f32
    ).astype(bf16)


def solution(mesh):
    placed = (P(("sp", "tp"), None), P(), P(), P(), P(), P(), P(), P("sp", "tp"), P())
    return jax.shard_map(
        per_device, mesh=mesh, in_specs=placed, out_specs=P(("sp", "tp"), None), check_vma=False
    )
```

```python
from functools import partial
import math

import jax
import jax.numpy as jnp
from jax import lax
from jax.experimental import pallas as pl
from jax.experimental.pallas import tpu as pltpu
from jax.sharding import PartitionSpec as P

epsilon = 1e-06
LOG2E = math.log2(math.e)
SAFE_SCORE = 60.0
W = 256
LAG = 2
OUT_LAG = 2
MAX_STEPS = 16
VMEM_LIMIT = 24 * 2**20


def rms_norm(vector, gain_vec):
    return (
        vector * lax.rsqrt(jnp.mean(vector * vector, axis=-1, keepdims=True) + epsilon) * gain_vec
    )


def three_way(x):
    hi = x.astype(jnp.bfloat16)
    rest = x - hi.astype(jnp.float32)
    mid = rest.astype(jnp.bfloat16)
    lo = (rest - mid.astype(jnp.float32)).astype(jnp.bfloat16)
    return hi, mid, lo


class Plan:
    def __init__(self, sp, tp, rows, half, heads_dev, group_heads, head_size):
        self.sp, self.tp, self.rows, self.half = sp, tp, rows, half
        self.heads_dev, self.group_heads, self.head_size = heads_dev, group_heads, head_size
        self.tok = tp * rows
        self.side_cols = group_heads * rows
        self.tiles = 2 * self.side_cols // W
        self.n_key = self.tok // W
        self.dec_rows = 8 if 3 * heads_dev <= 6 else 16
        self.zs = sp // 2
        self.next, self.order = ring_next(self.zs)

    def group(self, scal):
        return scal[1] // self.half

    def member(self, scal):
        return lax.rem(scal[1], self.half)

    def chunk_of(self, scal, j, hf):
        member = lax.rem(self.member(scal) - j + self.half, self.half)
        group = self.group(scal)
        return member + jnp.where(hf == 0, group, 1 - group) * self.half

    def side_chunk(self, scal, side):
        group = self.group(scal)
        return self.member(scal) + jnp.where(side == 0, 1 - group, group) * self.half

    def block_of(self, scal, k, yy):
        z, y = scal[0] // 2, lax.rem(scal[0], 2)
        source = jnp.int32(0)
        for zz in range(self.zs):
            value = self.order[(self.order.index(zz) - k) % self.zs]
            source = jnp.where(z == zz, value, source)
        return source * 2 + (y if yy == 0 else 1 - y)


def build_keys(plan, scal, kv_refs, keys, vals, row0):
    rows, half, dh = plan.rows, plan.half, plan.head_size
    f32, bf16 = jnp.float32, jnp.bfloat16
    per_piece = 2 * rows // 128
    pad = jnp.zeros((128 - dh - half * plan.dec_rows, 128), f32)
    for u in range(plan.tok // 128):
        j, v = u // per_piece, u % per_piece
        chunk = plan.chunk_of(scal, j, v * 128 // rows)
        dec = 2 * rows + (chunk * (rows // 128) + v % (rows // 128)) * 16
        dec = pl.multiple_of(dec, 16)
        kv = kv_refs[j][v * 128 : (v + 1) * 128, :]
        kv_t = kv.T
        gates = [r[pl.ds(dec, 16), :].astype(f32)[: plan.dec_rows] for r in kv_refs]
        extra = jnp.concatenate([kv_t[:dh].astype(f32)] + gates + [pad], axis=0)
        dst = row0 + u * 128
        keys[dst : dst + 128, :128] = kv
        keys[dst : dst + 128, 128:] = extra.T.astype(bf16)
        vals[:, dst : dst + 128] = kv_t[dh:]


def build_queries(plan, scal, q_refs, kv_refs, qs):
    rows, half, dh, hd, dr = plan.rows, plan.half, plan.head_size, plan.heads_dev, plan.dec_rows
    f32, bf16 = jnp.float32, jnp.bfloat16
    row = lax.broadcasted_iota(jnp.int32, (half * dr, rows), 0)
    part = row % dr
    for side in range(2):
        chunk = plan.side_chunk(scal, side)
        own = []
        for r in kv_refs:
            first = 2 * rows + chunk * (rows // 128) * 16
            own.append(
                jnp.concatenate(
                    [
                        r[pl.ds(pl.multiple_of(first + v * 16, 16), 16), :].astype(f32)
                        for v in range(rows // 128)
                    ],
                    axis=1,
                )
            )
        for h in range(plan.group_heads):
            q = q_refs[side][h * dh : (h + 1) * dh, :].astype(f32) * (LOG2E * dh**-0.5)
            q_hi = q.astype(bf16)
            q_lo = (q - q_hi.astype(f32)).astype(bf16)
            piece, i = lax.rem(plan.member(scal) - h // hd + half, half), h % hd
            tail = jnp.where((row // dr == piece) & (part < 3 * hd) & (part % hd == i), -1.0, 0.0)
            for e, at in enumerate((3 * hd, 3 * hd + 1, dr + 3 * hd)):
                gate = sum(
                    jnp.where(piece == j, o[e * hd + i : e * hd + i + 1], 0.0)
                    for j, o in enumerate(own)
                )
                tail = jnp.where(row == at, gate, tail)
            flat = (side * plan.group_heads + h) * rows
            n, lane = flat // W, flat % W
            sl = slice(lane, lane + rows)
            qs[n, 0:64, sl] = q_hi
            qs[n, 64:128, sl] = jnp.zeros((64, rows), bf16)
            qs[n, 128:192, sl] = q_lo
            qs[n, 192 : 192 + half * dr, sl] = tail.astype(bf16)
            qs[n, 192 + half * dr :, sl] = jnp.zeros((64 - half * dr, rows), bf16)


def attend_call(plan, opts, *refs):
    blocks, first, last, tile0, tile1, max_steps = opts
    n_blocks = len(blocks)
    half, rows, dh, n_key = plan.half, plan.rows, plan.head_size, plan.n_key
    f32, bf16 = jnp.float32, jnp.bfloat16
    refs = list(refs)
    scal = refs.pop(0)
    unsafe = refs.pop(0)[0]
    kv_refs = [[refs.pop(0) for _ in range(half)] for _ in range(n_blocks)]
    if first:
        q_refs = [refs.pop(0), refs.pop(0)]
    else:
        qs, acc_in, tot_in, peak_in = [refs.pop(0) for _ in range(4)]
    if first:
        qs, acc, tot, peak = [refs.pop(0) for _ in range(4)]
    elif not last:
        acc, tot, peak = [refs.pop(0) for _ in range(3)]
    else:
        out = refs.pop(0)
        acc, tot, peak = [refs.pop(0) for _ in range(3)]
    keys, vals = refs
    n_tiles = tile1 - tile0

    if first:
        acc[...] = jnp.zeros_like(acc)
        tot[...] = jnp.zeros_like(tot)
        peak[...] = jnp.full(peak.shape, -1e30, f32)
    elif last:
        acc[...] = acc_in[tile0:tile1]
        tot[...] = tot_in[tile0:tile1]
        peak[...] = peak_in[tile0:tile1]

    def build():
        for b in range(n_blocks):
            build_keys(plan, scal, kv_refs[b], keys, vals, b * plan.tok)

    def key_pos(kb):
        flat = kb * W + lax.broadcasted_iota(jnp.int32, (W, 1), 0)
        piece = flat // rows
        member = lax.rem(plan.member(scal) - piece // 2 + half, half)
        group = plan.group(scal)
        side = jnp.where(lax.rem(piece, 2) == 0, group, 1 - group)
        return (member + side * half) * rows + lax.rem(flat, rows)

    def query_pos(n):
        flat = lax.rem(n * W, plan.side_cols) + lax.broadcasted_iota(jnp.int32, (1, W), 1)
        side = jnp.where(n * W >= plan.side_cols, 1, 0)
        return plan.side_chunk(scal, side) * rows + lax.rem(flat, rows)

    def scoped(*accs):
        ring = LAG + 1
        per = ring + 2
        s_acc = [accs[m * per : m * per + ring] for m in range(2)]
        o_acc = [accs[m * per + ring : m * per + per] for m in range(2)]
        pairs = n_tiles // 2
        n_kb = n_blocks * n_key

        def group(first_pair, count):
            steps = [(p, kb) for p in range(count) for kb in range(n_kb)]

            def front(n):
                p, kb = steps[n]
                kk = keys[kb * W : (kb + 1) * W, :]
                for m in range(2):
                    tile = tile0 + 2 * (first_pair + p) + m
                    pltpu.matmul_push_rhs(qs[tile], staging_register=0, mxu_index=m)
                    pltpu.matmul_acc_lhs(s_acc[m][n % ring], kk, load_staged_rhs=0)

            def back(n):
                p, kb = steps[n]
                vt = vals[:, kb * W : (kb + 1) * W]
                for m in range(2):
                    tile = 2 * (first_pair + p) + m
                    e = jnp.exp2(pltpu.matmul_pop(s_acc[m][n % ring]))
                    if first:
                        e = jnp.where(key_pos(kb) <= query_pos(tile0 + tile), e, 0.0)
                    tot[tile] += jnp.sum(e.reshape(W // 8, 8, W), axis=0)
                    pltpu.matmul_push_rhs(e.astype(bf16), staging_register=1, mxu_index=m)
                    pltpu.matmul_acc_lhs(o_acc[m][p % 2], vt, load_staged_rhs=1)

            def finish(n):
                p, kb = steps[n]
                if kb == n_kb - 1:
                    for m in range(2):
                        acc[2 * (first_pair + p) + m] += pltpu.matmul_pop(o_acc[m][p % 2])

            total = len(steps)
            for n in range(total + LAG + OUT_LAG):
                if n < total:
                    front(n)
                if LAG <= n < total + LAG:
                    back(n - LAG)
                if n >= LAG + OUT_LAG:
                    finish(n - LAG - OUT_LAG)

        def fast():
            build()
            count = max(1, min(pairs, max_steps // n_kb))
            while pairs % count:
                count -= 1
            if count == pairs:
                group(0, pairs)
            else:

                def trip(i, carry):
                    group(i * count, count)
                    return carry

                lax.fori_loop(0, pairs // count, trip, 0)

        def slow():
            build()

            def tile_loop(n, carry):
                def block_loop(kb, carry):
                    off = pl.multiple_of(kb * W, W)
                    pltpu.matmul_push_rhs(qs[tile0 + n], staging_register=0, mxu_index=0)
                    pltpu.matmul_acc_lhs(s_acc[0][0], keys[pl.ds(off, W), :], load_staged_rhs=0)
                    s = pltpu.matmul_pop(s_acc[0][0])
                    if first:
                        seen = key_pos(kb) <= query_pos(tile0 + n)
                        s = jnp.where(seen, s, -1e30)
                    new = jnp.maximum(peak[n], jnp.max(s, axis=0, keepdims=True))
                    e = jnp.exp2(s - new)
                    if first:
                        e = jnp.where(seen, e, 0.0)
                    scale = jnp.exp2(peak[n] - new)
                    peak[n] = new
                    tot[n] = tot[n] * scale + jnp.sum(e.reshape(W // 8, 8, W), axis=0)
                    pltpu.matmul_push_rhs(e.astype(bf16), staging_register=1, mxu_index=0)
                    pltpu.matmul_acc_lhs(o_acc[0][0], vals[:, pl.ds(off, W)], load_staged_rhs=1)
                    acc[n] = acc[n] * scale + pltpu.matmul_pop(o_acc[0][0])
                    return carry

                return lax.fori_loop(0, n_kb, block_loop, carry)

            lax.fori_loop(0, n_tiles, tile_loop, 0)

        if first:
            build_queries(plan, scal, q_refs, kv_refs[0], qs)
            pl.when(unsafe == 0)(fast)
            pl.when(unsafe != 0)(slow)
        else:
            seen_block = plan.block_of(scal, *blocks[0]) < scal[0]
            pl.when(seen_block & (unsafe == 0))(fast)
            pl.when(seen_block & (unsafe != 0))(slow)

    specs = []
    for m in range(2):
        specs += [pltpu.ACC(m)((W, W), f32)] * (LAG + 1) + [pltpu.ACC(m)((dh, W), f32)] * 2
    pl.run_scoped(scoped, *specs)

    if last:
        for n in range(n_tiles):
            value = (acc[n] / jnp.sum(tot[n], axis=0, keepdims=True)).astype(bf16)
            for v in range(W // rows):
                flat = n * W + v * rows
                h = flat // rows
                out[h * dh : (h + 1) * dh, :] = value[:, v * rows : (v + 1) * rows]


def attend(plan, blocks, scal, unsafe, kv, state, first, last, tiles, max_steps):
    tile0, tile1 = tiles
    n, dh = plan.tiles, plan.head_size
    bf16, f32 = jnp.bfloat16, jnp.float32
    vmem = pl.BlockSpec(memory_space=pltpu.VMEM)
    sums = [
        jax.ShapeDtypeStruct((n, dh, W), f32),
        jax.ShapeDtypeStruct((n, 8, W), f32),
        jax.ShapeDtypeStruct((n, 1, W), f32),
    ]
    count = tile1 - tile0
    scratch = [
        pltpu.VMEM((len(blocks) * plan.tok, W), bf16),
        pltpu.VMEM((dh, len(blocks) * plan.tok), bf16),
    ]
    operands = [scal, unsafe] + [p for b in kv for p in b] + list(state)
    aliases = {}
    if first:
        out_shape = [jax.ShapeDtypeStruct((n, W, W), bf16)] + sums
    elif not last:
        out_shape = sums
        aliases = {len(operands) - 3 + i: i for i in range(3)}
    else:
        out_shape = [jax.ShapeDtypeStruct((plan.group_heads * dh, plan.rows), bf16)]
        scratch = [
            pltpu.VMEM((count, dh, W), f32),
            pltpu.VMEM((count, 8, W), f32),
            pltpu.VMEM((count, 1, W), f32),
        ] + scratch
    cells = count * W * len(blocks) * plan.tok
    return pl.pallas_call(
        partial(attend_call, plan, (blocks, first, last, tile0, tile1, max_steps)),
        out_shape=out_shape,
        in_specs=[pl.BlockSpec(memory_space=pltpu.SMEM)] * 2 + [vmem] * (len(operands) - 2),
        out_specs=[vmem] * len(out_shape),
        scratch_shapes=scratch,
        input_output_aliases=aliases,
        compiler_params=pltpu.CompilerParams(vmem_limit_bytes=VMEM_LIMIT),
        cost_estimate=pl.CostEstimate(
            flops=16 * cells * W, bytes_accessed=2**20, transcendentals=cells
        ),
        name="attend",
    )(*operands)


def project_kernel(half, scal, x, in_gain, w_key, w_value, key_gain, q_gain, gates, *outs):
    normed, mine, theirs, dec, unsafe = outs
    f32, bf16 = jnp.float32, jnp.bfloat16
    rows, dh, heads_dev = x.shape[0], key_gain.shape[1] // 2, gates.shape[0]
    rows_in = x[...].astype(f32)
    scale = lax.rsqrt(jnp.mean(rows_in * rows_in, axis=1, keepdims=True) + epsilon)
    normed[...] = (rows_in * scale * in_gain[...]).astype(bf16)
    key = jnp.dot(normed[...], w_key[...], preferred_element_type=f32)
    value = jnp.dot(normed[...], w_value[...], preferred_element_type=f32).astype(bf16)
    low = lax.broadcasted_iota(jnp.int32, key.shape, 1) < dh
    square = key * key
    mean0 = jnp.sum(jnp.where(low, square, 0.0), axis=1, keepdims=True) * (1.0 / dh)
    mean1 = jnp.sum(jnp.where(low, 0.0, square), axis=1, keepdims=True) * (1.0 / dh)
    scale = jnp.where(low, lax.rsqrt(mean0 + epsilon), lax.rsqrt(mean1 + epsilon))
    key = (key * scale * key_gain[...]).astype(bf16)
    head0 = jnp.concatenate([key[:, :dh], value[:, :dh]], axis=1)
    head1 = jnp.concatenate([key[:, dh:], value[:, dh:]], axis=1)
    first = scal[1] < half
    mine[...] = jnp.where(first, head0, head1)
    theirs[...] = jnp.where(first, head1, head0)
    parts = [p.astype(f32) for p in three_way(gates[...] * LOG2E)]
    spare = jnp.ones((16 - 3 * heads_dev, 128), f32)
    for b in range(gates.shape[1] // 128):
        sl = slice(b * 128, (b + 1) * 128)
        dec[b * 16 : (b + 1) * 16, :] = jnp.concatenate(
            [p[:, sl] for p in parts] + [spare], axis=0
        ).astype(bf16)
    bound = jnp.max(q_gain[...] * key_gain[...]) * (dh**0.5 * 1.02)
    unsafe[0] = jnp.where(bound <= SAFE_SCORE, 0, 1).astype(jnp.int32)


def query_kernel(half, own, scal, normed, w_query, gain, out):
    f32 = jnp.float32
    width, dh = out.shape[0], gain.shape[0]
    first = (scal[1] < half) == own
    start = pl.multiple_of(jnp.where(first, 0, width), 128)
    q = jnp.dot(normed[...], w_query[:, pl.ds(start, width)], preferred_element_type=f32)
    q = q.T
    for h in range(width // dh):
        one = q[h * dh : (h + 1) * dh, :]
        scale = lax.rsqrt(jnp.mean(one * one, axis=0, keepdims=True) + epsilon)
        out[h * dh : (h + 1) * dh, :] = (one * scale * gain[...]).astype(out.dtype)


def output_kernel(half, own, scal, att, w_out, *refs):
    width = att.shape[0]
    first = (scal[1] < half) == own
    start = pl.multiple_of(jnp.where(first, 0, width), 128)
    share = lax.dot_general(
        att[...].T, w_out[pl.ds(start, width), :], (((1,), (0,)), ((), ())),
        preferred_element_type=jnp.float32,
    )
    if own:
        refs[0][...] = share
    else:
        refs[1][...] = (refs[0][...] + share).astype(refs[1].dtype)


def ring_next(count):
    order = [0] + list(range(1, count, 2)) + list(range((count - 1) // 2 * 2, 0, -2))
    return {order[i]: order[(i + 1) % count] for i in range(count)}, order


def per_device(inputs, in_gain, w_query, w_key, w_value, query_gain, key_gain, decay_sums, w_out):
    tp, sp = lax.axis_size("tp"), lax.axis_size("sp")
    s_rank, t_rank = lax.axis_index("sp"), lax.axis_index("tp")
    heads_dev = decay_sums.shape[1]
    head_size = query_gain.shape[0]
    kv_heads = w_key.shape[1] // head_size
    half = tp // kv_heads
    g_rank, c_rank = t_rank // half, t_rank % half
    group_heads = heads_dev * half
    rows = inputs.shape[0]
    tok = rows * tp
    bf16, f32 = jnp.bfloat16, jnp.float32
    axes = ("sp", "tp")
    zs = sp // 2

    def move(array, target):
        pairs = []
        for s in range(sp):
            for t in range(tp):
                s2, t2 = target(s, t)
                pairs.append((s * tp + t, s2 * tp + t2))
        return lax.ppermute(array, axes, pairs)

    nxt, _ = ring_next(zs)
    to_x = lambda s, t: (s, (t + half) % tp)
    to_y = lambda s, t: (s ^ 1, t)
    to_z = lambda s, t: (nxt[s // 2] * 2 + s % 2, t)

    def to_core(j):
        return lambda s, t: (s, t // half * half + (t % half + j) % half)

    scal = jnp.stack([s_rank, t_rank]).astype(jnp.int32)
    smem, vmem = pl.BlockSpec(memory_space=pltpu.SMEM), pl.BlockSpec(memory_space=pltpu.VMEM)
    width = group_heads * head_size
    depth = inputs.shape[1]
    params = pltpu.CompilerParams(vmem_limit_bytes=VMEM_LIMIT)

    def cost(flops):
        return pl.CostEstimate(flops=flops, bytes_accessed=2**20, transcendentals=0)

    two = lambda gain: jnp.concatenate([gain, gain]).reshape(1, -1)
    normed, mine, theirs, dec, unsafe = pl.pallas_call(
        partial(project_kernel, half),
        out_shape=[
            jax.ShapeDtypeStruct((rows, depth), bf16),
            jax.ShapeDtypeStruct((rows, 2 * head_size), bf16),
            jax.ShapeDtypeStruct((rows, 2 * head_size), bf16),
            jax.ShapeDtypeStruct((tok // 8, 128), bf16),
            jax.ShapeDtypeStruct((1,), jnp.int32),
        ],
        in_specs=[smem] + [vmem] * 7,
        out_specs=[vmem] * 4 + [smem],
        compiler_params=params,
        cost_estimate=cost(8 * rows * depth * W),
        name="project",
    )(
        scal,
        inputs,
        in_gain.reshape(1, -1),
        w_key,
        w_value,
        two(key_gain),
        two(query_gain),
        decay_sums.T,
    )
    recv = move(theirs, to_x)

    def project_queries(own):
        return pl.pallas_call(
            partial(query_kernel, half, own),
            out_shape=jax.ShapeDtypeStruct((width, rows), bf16),
            in_specs=[smem] + [vmem] * 3,
            out_specs=vmem,
            compiler_params=params,
            cost_estimate=cost(4 * rows * depth * width),
            name="queries",
        )(scal, normed, w_query, query_gain.reshape(-1, 1))

    q_recv = move(project_queries(False), to_x)
    own = jnp.concatenate([mine, recv, dec], axis=0)
    pieces = []
    for k in range(zs):
        if k:
            own = move(own, to_z)
        side = move(own, to_y)
        pieces.append(
            [[part] + [move(part, to_core(j)) for j in range(1, half)] for part in (own, side)]
        )
    q_own = project_queries(True)

    plan = Plan(sp, tp, rows, half, heads_dev, group_heads, head_size)

    def call(blocks, state, first=False, last=False, tiles=(0, plan.tiles), max_steps=MAX_STEPS):
        kv = [pieces[k][yy] for k, yy in blocks]
        return attend(plan, blocks, scal, unsafe, kv, state, first, last, tiles, max_steps)

    queries, *state = call([(0, 0)], (q_recv, q_own), first=True, max_steps=32)
    for k in range(zs - 1):
        if k < 2:
            if k:
                state = call([(k, 0)], (queries, *state))
            state = call([(k, 1)], (queries, *state))
        else:
            state = call([(k, 0), (k, 1)], (queries, *state))
    final = [(zs - 1, 0), (zs - 1, 1)]
    mid = plan.tiles // 2
    (att_other,) = call(final, (queries, *state), last=True, tiles=(0, mid), max_steps=32)
    back = move(att_other, to_x)
    (att_own,) = call(final, (queries, *state), last=True, tiles=(mid, plan.tiles), max_steps=32)

    def project_out(own, att, *share):
        kind = f32 if own else bf16
        return pl.pallas_call(
            partial(output_kernel, half, own),
            out_shape=jax.ShapeDtypeStruct((rows, w_out.shape[1]), kind),
            in_specs=[smem] + [vmem] * (2 + len(share)),
            out_specs=vmem,
            compiler_params=params,
            cost_estimate=cost(4 * rows * depth * width),
            name="output",
        )(scal, att, w_out, *share)

    return project_out(False, back, project_out(True, att_own))


def solution(mesh):
    placed = (P(("sp", "tp"), None), P(), P(), P(), P(), P(), P(), P("sp", "tp"), P())
    return jax.shard_map(
        per_device, mesh=mesh, in_specs=placed, out_specs=P(("sp", "tp"), None), check_vma=False
    )
```

```python
from functools import partial
import math

import jax
import jax.numpy as jnp
from jax import lax
from jax.experimental import pallas as pl
from jax.experimental.pallas import tpu as pltpu
from jax.sharding import PartitionSpec as P

epsilon = 1e-06
LOG2E = math.log2(math.e)
SAFE_SCORE = 60.0
W = 256
LAG = 2
OUT_LAG = 2
MAX_STEPS = 16
VMEM_LIMIT = 24 * 2**20


def rms_norm(vector, gain_vec):
    return (
        vector * lax.rsqrt(jnp.mean(vector * vector, axis=-1, keepdims=True) + epsilon) * gain_vec
    )


def three_way(x):
    hi = x.astype(jnp.bfloat16)
    rest = x - hi.astype(jnp.float32)
    mid = rest.astype(jnp.bfloat16)
    lo = (rest - mid.astype(jnp.float32)).astype(jnp.bfloat16)
    return hi, mid, lo


class Plan:
    def __init__(self, sp, tp, rows, half, heads_dev, group_heads, head_size):
        self.sp, self.tp, self.rows, self.half = sp, tp, rows, half
        self.heads_dev, self.group_heads, self.head_size = heads_dev, group_heads, head_size
        self.tok = tp * rows
        self.side_cols = group_heads * rows
        self.tiles = 2 * self.side_cols // W
        self.n_key = self.tok // W
        self.dec_rows = 16
        self.zs = sp // 2
        self.next, self.order = ring_next(self.zs)

    def group(self, scal):
        return scal[1] // self.half

    def member(self, scal):
        return lax.rem(scal[1], self.half)

    def chunk_of(self, scal, j, hf):
        member = lax.rem(self.member(scal) - j + self.half, self.half)
        group = self.group(scal)
        return member + jnp.where(hf == 0, group, 1 - group) * self.half

    def side_chunk(self, scal, side):
        group = self.group(scal)
        return self.member(scal) + jnp.where(side == 0, 1 - group, group) * self.half

    def block_of(self, scal, k, yy):
        z, y = scal[0] // 2, lax.rem(scal[0], 2)
        source = jnp.int32(0)
        for zz in range(self.zs):
            value = self.order[(self.order.index(zz) - k) % self.zs]
            source = jnp.where(z == zz, value, source)
        return source * 2 + (y if yy == 0 else 1 - y)


def build_keys(plan, scal, kv_refs, keys, vals, row0, rolled):
    rows, half, dh = plan.rows, plan.half, plan.head_size
    f32, bf16 = jnp.float32, jnp.bfloat16
    per_piece = 2 * rows // 128
    spare = 128 - dh - half * 16
    pad = [jnp.zeros((spare, 128), bf16)] if spare else []

    def part(j, v, u):
        if isinstance(v, int):
            hf, off = v * 128 // rows, v % (rows // 128)
        else:
            hf, off = v * 128 // rows, lax.rem(v, rows // 128)
        chunk = plan.chunk_of(scal, j, hf)
        dec = pl.multiple_of(2 * rows + (chunk * (rows // 128) + off) * 16, 16)
        kv = kv_refs[j][pl.ds(v * 128, 128), :]
        kv_t = kv.T
        extra = jnp.concatenate(
            [kv_t[:dh]] + [r[pl.ds(dec, 16), :] for r in kv_refs] + pad, axis=0
        )
        dst = row0 + u * 128
        keys[pl.ds(dst, 128), :128] = kv
        keys[pl.ds(dst, 128), 128:] = extra.T
        vals[:, pl.ds(dst, 128)] = kv_t[dh:]

    for j in range(half):
        if rolled:

            def step(v, carry, j=j):
                v = pl.multiple_of(v, 1)
                part(j, v, j * per_piece + v)
                return carry

            lax.fori_loop(0, per_piece, step, 0)
        else:
            for v in range(per_piece):
                part(j, v, j * per_piece + v)


def build_queries(plan, scal, q_refs, kv_refs, qs):
    rows, half, dh, hd, dr = plan.rows, plan.half, plan.head_size, plan.heads_dev, plan.dec_rows
    f32, bf16 = jnp.float32, jnp.bfloat16
    row = lax.broadcasted_iota(jnp.int32, (half * dr, rows), 0)
    part = row % dr
    for side in range(2):
        chunk = plan.side_chunk(scal, side)
        own = []
        for r in kv_refs:
            first = 2 * rows + chunk * (rows // 128) * 16
            own.append(
                jnp.concatenate(
                    [
                        r[pl.ds(pl.multiple_of(first + v * 16, 16), 16), :].astype(f32)
                        for v in range(rows // 128)
                    ],
                    axis=1,
                )
            )
        for h in range(plan.group_heads):
            q = q_refs[side][h * dh : (h + 1) * dh, :].astype(f32) * (LOG2E * dh**-0.5)
            q_hi = q.astype(bf16)
            q_lo = (q - q_hi.astype(f32)).astype(bf16)
            piece, i = lax.rem(plan.member(scal) - h // hd + half, half), h % hd
            tail = jnp.where((row // dr == piece) & (part < 3 * hd) & (part % hd == i), -1.0, 0.0)
            for e, at in enumerate((3 * hd, 3 * hd + 1, dr + 3 * hd)):
                gate = sum(
                    jnp.where(piece == j, o[e * hd + i : e * hd + i + 1], 0.0)
                    for j, o in enumerate(own)
                )
                tail = jnp.where(row == at, gate, tail)
            flat = (side * plan.group_heads + h) * rows
            n, lane = flat // W, flat % W
            sl = slice(lane, lane + rows)
            qs[n, 0:64, sl] = q_hi
            qs[n, 64:128, sl] = jnp.zeros((64, rows), bf16)
            qs[n, 128:192, sl] = q_lo
            qs[n, 192 : 192 + half * dr, sl] = tail.astype(bf16)
            if half * dr < 64:
                qs[n, 192 + half * dr :, sl] = jnp.zeros((64 - half * dr, rows), bf16)


def attend_call(plan, opts, *refs):
    blocks, first, last, tile0, tile1, max_steps = opts
    n_blocks = len(blocks)
    half, rows, dh, n_key = plan.half, plan.rows, plan.head_size, plan.n_key
    f32, bf16 = jnp.float32, jnp.bfloat16
    refs = list(refs)
    scal = (lax.axis_index("sp"), lax.axis_index("tp"))
    unsafe = jnp.max(refs.pop(0)[...])
    kv_refs = [[refs.pop(0) for _ in range(half)] for _ in range(n_blocks)]
    if first:
        q_refs = [refs.pop(0), refs.pop(0)]
    else:
        qs, acc_in, tot_in, peak_in = [refs.pop(0) for _ in range(4)]
    if first:
        qs, acc, tot, peak = [refs.pop(0) for _ in range(4)]
    elif not last:
        acc, tot, peak = [refs.pop(0) for _ in range(3)]
    else:
        out = refs.pop(0)
        acc, tot, peak = [refs.pop(0) for _ in range(3)]
    keys, vals = refs
    n_tiles = tile1 - tile0

    if first:
        acc[...] = jnp.zeros_like(acc)
        tot[...] = jnp.zeros_like(tot)
        peak[...] = jnp.full(peak.shape, -1e30, f32)
    elif last:
        acc[...] = acc_in[tile0:tile1]
        tot[...] = tot_in[tile0:tile1]
        peak[...] = peak_in[tile0:tile1]

    def build(rolled):
        for b in range(n_blocks):
            build_keys(plan, scal, kv_refs[b], keys, vals, b * plan.tok, rolled)

    def key_pos(kb):
        flat = kb * W + lax.broadcasted_iota(jnp.int32, (W, 1), 0)
        piece = flat // rows
        member = lax.rem(plan.member(scal) - piece // 2 + half, half)
        group = plan.group(scal)
        side = jnp.where(lax.rem(piece, 2) == 0, group, 1 - group)
        return (member + side * half) * rows + lax.rem(flat, rows)

    def mask(e, kb, n):
        pos = query_pos(n)
        step = min(rows, W)
        parts = []
        for r in range(0, W, step):
            flat = kb * W + r
            piece = flat // rows
            base = plan.chunk_of(scal, piece // 2, piece % 2) * rows + flat % rows
            seen = lax.broadcasted_iota(jnp.int32, (step, W), 0) <= pos - base
            parts.append(jnp.where(seen, e[r : r + step], 0.0))
        return jnp.concatenate(parts, axis=0) if len(parts) > 1 else parts[0]

    def query_pos(n):
        flat = lax.rem(n * W, plan.side_cols) + lax.broadcasted_iota(jnp.int32, (1, W), 1)
        side = jnp.where(n * W >= plan.side_cols, 1, 0)
        return plan.side_chunk(scal, side) * rows + lax.rem(flat, rows)

    def scoped(*accs):
        ring = LAG + 1
        per = ring + 2
        s_acc = [accs[m * per : m * per + ring] for m in range(2)]
        o_acc = [accs[m * per + ring : m * per + per] for m in range(2)]
        pairs = n_tiles // 2
        n_kb = n_blocks * n_key

        def group(first_pair, count):
            steps = [(p, kb) for p in range(count) for kb in range(n_kb)]

            def front(n):
                p, kb = steps[n]
                kk = keys[kb * W : (kb + 1) * W, :]
                for m in range(2):
                    tile = tile0 + 2 * (first_pair + p) + m
                    pltpu.matmul_push_rhs(qs[tile], staging_register=0, mxu_index=m)
                    pltpu.matmul_acc_lhs(s_acc[m][n % ring], kk, load_staged_rhs=0)

            def back(n):
                p, kb = steps[n]
                vt = vals[:, kb * W : (kb + 1) * W]
                for m in range(2):
                    tile = 2 * (first_pair + p) + m
                    e = jnp.exp2(pltpu.matmul_pop(s_acc[m][n % ring]))
                    if first:
                        e = mask(e, kb, tile0 + tile)
                    tot[tile] += jnp.sum(e.reshape(W // 8, 8, W), axis=0)
                    pltpu.matmul_push_rhs(e.astype(bf16), staging_register=1, mxu_index=m)
                    pltpu.matmul_acc_lhs(o_acc[m][p % 2], vt, load_staged_rhs=1)

            def finish(n):
                p, kb = steps[n]
                if kb == n_kb - 1:
                    for m in range(2):
                        acc[2 * (first_pair + p) + m] += pltpu.matmul_pop(o_acc[m][p % 2])

            total = len(steps)
            for n in range(total + LAG + OUT_LAG):
                if n < total:
                    front(n)
                if LAG <= n < total + LAG:
                    back(n - LAG)
                if n >= LAG + OUT_LAG:
                    finish(n - LAG - OUT_LAG)

        def fast():
            build(False)
            count = max(1, min(pairs, max_steps // n_kb))
            while pairs % count:
                count -= 1
            if count == pairs:
                group(0, pairs)
            else:

                def trip(i, carry):
                    group(i * count, count)
                    return carry

                lax.fori_loop(0, pairs // count, trip, 0)

        def slow():
            build(True)

            def tile_loop(n, carry):
                def block_loop(kb, carry):
                    off = pl.multiple_of(kb * W, W)
                    pltpu.matmul_push_rhs(qs[tile0 + n], staging_register=0, mxu_index=0)
                    pltpu.matmul_acc_lhs(s_acc[0][0], keys[pl.ds(off, W), :], load_staged_rhs=0)
                    s = pltpu.matmul_pop(s_acc[0][0])
                    if first:
                        seen = key_pos(kb) <= query_pos(tile0 + n)
                        s = jnp.where(seen, s, -1e30)
                    new = jnp.maximum(peak[n], jnp.max(s, axis=0, keepdims=True))
                    e = jnp.exp2(s - new)
                    if first:
                        e = jnp.where(seen, e, 0.0)
                    scale = jnp.exp2(peak[n] - new)
                    peak[n] = new
                    tot[n] = tot[n] * scale + jnp.sum(e.reshape(W // 8, 8, W), axis=0)
                    pltpu.matmul_push_rhs(e.astype(bf16), staging_register=1, mxu_index=0)
                    pltpu.matmul_acc_lhs(o_acc[0][0], vals[:, pl.ds(off, W)], load_staged_rhs=1)
                    acc[n] = acc[n] * scale + pltpu.matmul_pop(o_acc[0][0])
                    return carry

                return lax.fori_loop(0, n_kb, block_loop, carry)

            lax.fori_loop(0, n_tiles, tile_loop, 0)

        if first:
            build_queries(plan, scal, q_refs, kv_refs[0], qs)
            pl.when(unsafe == 0.0)(fast)
            pl.when(unsafe != 0.0)(slow)
        else:
            seen_block = plan.block_of(scal, *blocks[0]) < scal[0]
            pl.when(seen_block & (unsafe == 0.0))(fast)
            pl.when(seen_block & (unsafe != 0.0))(slow)

    specs = []
    for m in range(2):
        specs += [pltpu.ACC(m)((W, W), f32)] * (LAG + 1) + [pltpu.ACC(m)((dh, W), f32)] * 2
    pl.run_scoped(scoped, *specs)

    if last:
        for n in range(n_tiles):
            value = (acc[n] / jnp.sum(tot[n], axis=0, keepdims=True)).astype(bf16)
            for v in range(W // rows):
                flat = n * W + v * rows
                h = flat // rows
                out[h * dh : (h + 1) * dh, :] = value[:, v * rows : (v + 1) * rows]


def attend(plan, blocks, unsafe, kv, state, first, last, tiles, max_steps):
    tile0, tile1 = tiles
    n, dh = plan.tiles, plan.head_size
    bf16, f32 = jnp.bfloat16, jnp.float32
    vmem = pl.BlockSpec(memory_space=pltpu.VMEM)
    sums = [
        jax.ShapeDtypeStruct((n, dh, W), f32),
        jax.ShapeDtypeStruct((n, 8, W), f32),
        jax.ShapeDtypeStruct((n, 1, W), f32),
    ]
    count = tile1 - tile0
    scratch = [
        pltpu.VMEM((len(blocks) * plan.tok, W), bf16),
        pltpu.VMEM((dh, len(blocks) * plan.tok), bf16),
    ]
    operands = [unsafe] + [p for b in kv for p in b] + list(state)
    aliases = {}
    if first:
        out_shape = [jax.ShapeDtypeStruct((n, W, W), bf16)] + sums
    elif not last:
        out_shape = sums
        aliases = {len(operands) - 3 + i: i for i in range(3)}
    else:
        out_shape = [jax.ShapeDtypeStruct((plan.group_heads * dh, plan.rows), bf16)]
        scratch = [
            pltpu.VMEM((count, dh, W), f32),
            pltpu.VMEM((count, 8, W), f32),
            pltpu.VMEM((count, 1, W), f32),
        ] + scratch
    cells = count * W * len(blocks) * plan.tok
    return pl.pallas_call(
        partial(attend_call, plan, (blocks, first, last, tile0, tile1, max_steps)),
        out_shape=out_shape,
        in_specs=[vmem] * len(operands),
        out_specs=[vmem] * len(out_shape),
        scratch_shapes=scratch,
        input_output_aliases=aliases,
        compiler_params=pltpu.CompilerParams(vmem_limit_bytes=VMEM_LIMIT),
        cost_estimate=pl.CostEstimate(
            flops=16 * cells * W, bytes_accessed=2**20, transcendentals=cells
        ),
        name="attend",
    )(*operands)


def project_kernel(half, *refs):
    x_h, gain_h, key_h, value_h, key_gain_h, q_gain_h, gates_h, query_h = refs[:8]
    normed, mine, theirs, dec, unsafe, w_query = refs[8:14]
    x, in_gain, w_key, w_value, key_gain, q_gain, gates, sems = refs[14:]
    copies = [
        pltpu.make_async_copy(src, dst, sems.at[n])
        for n, (src, dst) in enumerate(
            (
                (x_h, x),
                (gain_h, in_gain),
                (key_h, w_key),
                (value_h, w_value),
                (key_gain_h, key_gain),
                (q_gain_h, q_gain),
                (gates_h, gates),
                (query_h, w_query),
            )
        )
    ]
    for copy in copies:
        copy.start()
    for copy in copies[:2]:
        copy.wait()
    f32, bf16 = jnp.float32, jnp.bfloat16
    rows, dh, heads_dev = x.shape[0], key_gain.shape[1], gates.shape[0]
    rows_in = x[...].astype(f32)
    scale = lax.rsqrt(jnp.mean(rows_in * rows_in, axis=1, keepdims=True) + epsilon)
    normed[...] = (rows_in * scale * in_gain[...]).astype(bf16)
    for copy in copies[2:6]:
        copy.wait()
    key = jnp.dot(normed[...], w_key[...], preferred_element_type=f32)
    value = jnp.dot(normed[...], w_value[...], preferred_element_type=f32).astype(bf16)
    low = lax.broadcasted_iota(jnp.int32, key.shape, 1) < dh
    square = key * key
    mean0 = jnp.sum(jnp.where(low, square, 0.0), axis=1, keepdims=True) * (1.0 / dh)
    mean1 = jnp.sum(jnp.where(low, 0.0, square), axis=1, keepdims=True) * (1.0 / dh)
    scale = jnp.where(low, lax.rsqrt(mean0 + epsilon), lax.rsqrt(mean1 + epsilon))
    both = jnp.concatenate([key_gain[...], key_gain[...]], axis=1)
    key = (key * scale * both).astype(bf16)
    head0 = jnp.concatenate([key[:, :dh], value[:, :dh]], axis=1)
    head1 = jnp.concatenate([key[:, dh:], value[:, dh:]], axis=1)
    first = lax.axis_index("tp") < half
    mine[...] = jnp.where(first, head0, head1)
    theirs[...] = jnp.where(first, head1, head0)
    copies[6].wait()
    parts = [p.astype(f32) for p in three_way(gates[...] * LOG2E)]
    spare = jnp.ones((16 - 3 * heads_dev, 128), f32)
    for b in range(gates.shape[1] // 128):
        sl = slice(b * 128, (b + 1) * 128)
        dec[b * 16 : (b + 1) * 16, :] = jnp.concatenate(
            [p[:, sl] for p in parts] + [spare], axis=0
        ).astype(bf16)
    bound = jnp.max(q_gain[...] * key_gain[...]) * (dh**0.5 * 1.02)
    unsafe[...] = jnp.full(unsafe.shape, jnp.where(bound <= SAFE_SCORE, 0.0, 1.0), f32)
    copies[7].wait()


def query_kernel(half, own, normed, w_query, gain, out):
    f32 = jnp.float32
    width, dh = out.shape[0], gain.shape[1]
    column = jnp.broadcast_to(gain[...], (8, dh)).T[:, :1]
    first = (lax.axis_index("tp") < half) == own
    start = pl.multiple_of(jnp.where(first, 0, width), 128)
    q = jnp.dot(normed[...], w_query[:, pl.ds(start, width)], preferred_element_type=f32)
    q = q.T
    for h in range(width // dh):
        one = q[h * dh : (h + 1) * dh, :]
        scale = lax.rsqrt(jnp.mean(one * one, axis=0, keepdims=True) + epsilon)
        out[h * dh : (h + 1) * dh, :] = (one * scale * column).astype(out.dtype)


def output_kernel(half, own, att, w_out, *refs):
    width = att.shape[0]
    first = (lax.axis_index("tp") < half) == own
    start = pl.multiple_of(jnp.where(first, 0, width), 128)
    share = lax.dot_general(
        att[...].T, w_out[pl.ds(start, width), :], (((1,), (0,)), ((), ())),
        preferred_element_type=jnp.float32,
    )
    if own:
        refs[0][...] = share
    else:
        refs[1][...] = (refs[0][...] + share).astype(refs[1].dtype)


def ring_next(count):
    order = [0] + list(range(1, count, 2)) + list(range((count - 1) // 2 * 2, 0, -2))
    return {order[i]: order[(i + 1) % count] for i in range(count)}, order


def per_device(inputs, in_gain, w_query, w_key, w_value, query_gain, key_gain, decay_sums, w_out):
    tp, sp = lax.axis_size("tp"), lax.axis_size("sp")
    s_rank, t_rank = lax.axis_index("sp"), lax.axis_index("tp")
    heads_dev = decay_sums.shape[1]
    head_size = query_gain.shape[0]
    kv_heads = w_key.shape[1] // head_size
    half = tp // kv_heads
    g_rank, c_rank = t_rank // half, t_rank % half
    group_heads = heads_dev * half
    rows = inputs.shape[0]
    tok = rows * tp
    bf16, f32 = jnp.bfloat16, jnp.float32
    axes = ("sp", "tp")
    zs = sp // 2

    def move(array, target):
        pairs = []
        for s in range(sp):
            for t in range(tp):
                s2, t2 = target(s, t)
                pairs.append((s * tp + t, s2 * tp + t2))
        return lax.ppermute(array, axes, pairs)

    nxt, _ = ring_next(zs)
    to_x = lambda s, t: (s, (t + half) % tp)
    to_y = lambda s, t: (s ^ 1, t)
    to_z = lambda s, t: (nxt[s // 2] * 2 + s % 2, t)

    def to_core(j):
        return lambda s, t: (s, t // half * half + (t % half + j) % half)

    vmem, hbm = pl.BlockSpec(memory_space=pltpu.VMEM), pl.BlockSpec(memory_space=pltpu.HBM)
    width = group_heads * head_size
    depth = inputs.shape[1]
    params = pltpu.CompilerParams(vmem_limit_bytes=VMEM_LIMIT)

    def cost(flops):
        return pl.CostEstimate(flops=flops, bytes_accessed=2**20, transcendentals=0)

    out_shape = [
        jax.ShapeDtypeStruct((rows, depth), bf16),
        jax.ShapeDtypeStruct((rows, 2 * head_size), bf16),
        jax.ShapeDtypeStruct((rows, 2 * head_size), bf16),
        jax.ShapeDtypeStruct((tok // 8, 128), bf16),
        jax.ShapeDtypeStruct((8, 128), f32),
        jax.ShapeDtypeStruct(w_query.shape, bf16),
    ]
    far = lambda a: pltpu.with_memory_space_constraint(a, pltpu.HBM)
    normed, mine, theirs, dec, unsafe, w_query = pl.pallas_call(
        partial(project_kernel, half),
        out_shape=out_shape,
        in_specs=[hbm] * 8,
        out_specs=[vmem] * len(out_shape),
        scratch_shapes=[
            pltpu.VMEM((rows, depth), bf16),
            pltpu.VMEM((1, depth), f32),
            pltpu.VMEM(w_key.shape, bf16),
            pltpu.VMEM(w_value.shape, bf16),
            pltpu.VMEM((1, head_size), f32),
            pltpu.VMEM((1, head_size), f32),
            pltpu.VMEM((heads_dev, tok), f32),
            pltpu.SemaphoreType.DMA((8,)),
        ],
        compiler_params=pltpu.CompilerParams(vmem_limit_bytes=VMEM_LIMIT),
        cost_estimate=cost(8 * rows * depth * W),
        name="project",
    )(
        far(inputs),
        far(in_gain.reshape(1, -1)),
        far(w_key),
        far(w_value),
        far(key_gain.reshape(1, -1)),
        far(query_gain.reshape(1, -1)),
        far(decay_sums.T),
        far(w_query),
    )
    recv = move(theirs, to_x)

    def project_queries(own):
        return pl.pallas_call(
            partial(query_kernel, half, own),
            out_shape=jax.ShapeDtypeStruct((width, rows), bf16),
            in_specs=[vmem] * 3,
            out_specs=vmem,
            compiler_params=params,
            cost_estimate=cost(4 * rows * depth * width),
            name="queries",
        )(normed, w_query, query_gain.reshape(1, -1))

    q_recv = move(project_queries(False), to_x)
    own = jnp.concatenate([mine, recv, dec], axis=0)
    pieces = []
    for k in range(zs):
        if k:
            own = move(own, to_z)
        side = move(own, to_y)
        pieces.append(
            [[part] + [move(part, to_core(j)) for j in range(1, half)] for part in (own, side)]
        )
    q_own = project_queries(True)

    plan = Plan(sp, tp, rows, half, heads_dev, group_heads, head_size)

    def call(blocks, state, first=False, last=False, tiles=(0, plan.tiles), max_steps=MAX_STEPS):
        kv = [pieces[k][yy] for k, yy in blocks]
        return attend(plan, blocks, unsafe, kv, state, first, last, tiles, max_steps)

    queries, *state = call([(0, 0)], (q_recv, q_own), first=True, max_steps=32)
    for k in range(zs - 1):
        if k < 2:
            if k:
                state = call([(k, 0)], (queries, *state))
            state = call([(k, 1)], (queries, *state))
        else:
            state = call([(k, 0), (k, 1)], (queries, *state))
    final = [(zs - 1, 0), (zs - 1, 1)]
    mid = plan.tiles // 2
    (att_other,) = call(final, (queries, *state), last=True, tiles=(0, mid), max_steps=32)
    back = move(att_other, to_x)
    (att_own,) = call(final, (queries, *state), last=True, tiles=(mid, plan.tiles), max_steps=32)

    def project_out(own, att, *share):
        kind = f32 if own else bf16
        return pl.pallas_call(
            partial(output_kernel, half, own),
            out_shape=jax.ShapeDtypeStruct((rows, w_out.shape[1]), kind),
            in_specs=[vmem] * (2 + len(share)),
            out_specs=vmem,
            compiler_params=params,
            cost_estimate=cost(4 * rows * depth * width),
            name="output",
        )(att, w_out, *share)

    return project_out(False, back, project_out(True, att_own))


def solution(mesh):
    placed = (P(("sp", "tp"), None), P(), P(), P(), P(), P(), P(), P("sp", "tp"), P())
    return jax.shard_map(
        per_device, mesh=mesh, in_specs=placed, out_specs=P(("sp", "tp"), None), check_vma=False
    )
```
